32 devices in a mesh: dp: 4 (over y, x), kv: 4 (over z), tp: 2 (over core).
Axes of the slice: x: 2, y: 2, z: 4, core: 2. Of those that a mesh axis runs over, the one named last changes fastest.
Arguments:
- tokens: bfloat16 [96, 2048], P('dp', 'kv'), may hold values from -6 to 6
- norm_gain: float32 [2048], P('kv'), may hold values from 0.1 to 1.9
- w_query: bfloat16 [2048, 1024], P('kv', 'tp'), may hold values from -0.125 to 0.125
- w_key: bfloat16 [2048, 256], P('kv', 'tp'), may hold values from -0.125 to 0.125
- w_value: bfloat16 [2048, 256], P('kv', 'tp'), may hold values from -0.125 to 0.125
- head_bias: float32 [8], P('tp'), may hold values from -1.5 to 1
- cache_key: bfloat16 [96, 2048, 2, 128], P('dp', 'kv', 'tp'), may hold values from -6 to 6
- cache_value: bfloat16 [96, 2048, 2, 128], P('dp', 'kv', 'tp'), may hold values from -6 to 6
- lengths: int32 [96], P('dp'), may hold values from 1 to 2047
- w_out: bfloat16 [1024, 2048], P('tp', 'kv'), may hold values from -0.1875 to 0.1875
Outputs:
- mixed: float32 [96, 2048], P('dp', 'kv')
- new_key: bfloat16 [96, 2, 128], P('dp', 'tp')
- new_value: bfloat16 [96, 2, 128], P('dp', 'tp')
The draws below stay inside these ranges and needn't reach their ends.
Inputs may be any that keep to these rules, and one draw needn't show every extreme that they name: `lengths`: each length lies between 1 and 2047, so that the new token has a place in the cache.
All inputs are finite; a program needn't handle non-finite values.
Results may differ from the reference program's by a relative error of at most 0.001.
Values sent between devices are 32-bit elements.
A program may use at most 64 MiB of HBM per device.

```python
import math
import jax
import jax.numpy as jnp
from jax import lax

D = 2048
HEADS = 8
KV_HEADS = 2
HEAD_DIM = 128
SEQS = 96
POS = 2048


def place_ends(array, stream_key, smallest, high):
    spot = [jax.random.randint(jax.random.fold_in(stream_key, axis), (), 0, length) for axis, length in enumerate(array.shape)]
    widest = array.shape.index(max(array.shape))
    neighbour = spot[:widest] + [(spot[widest] + 1) % array.shape[widest]] + spot[widest + 1:]
    return array.at[tuple(spot)].set(smallest).at[tuple(neighbour)].set(high)


def level_of(key, shape, cuts, low, high):
    gain = 1.0
    for position, blocks in cuts:
        heights = jax.random.uniform(jax.random.fold_in(jax.random.fold_in(key, 6), position), (blocks,), jnp.float32, low / len(cuts), high / len(cuts))
        gain = gain * jnp.repeat(jnp.exp(heights), shape[position] // blocks).reshape((-1,) + (1,) * (len(shape) - 1 - position))
    return gain


def gaussian(key, extent, scale, bound, split=(), kind=jnp.bfloat16):
    result = jax.random.normal(key, extent, jnp.float32) * scale
    if len(split) > 0:
        result = level_of(key, extent, split, -0.22, 0.18) * result
    return jnp.clip(result, min=-bound, max=bound).astype(kind)


def setup_inputs(seed: int = 0) -> dict:
    streams_of = jax.random.split(jax.random.key(seed), 11)
    return {
        "tokens": gaussian(streams_of[0], (SEQS, D), 1.0, 6.0, ((0, 4), (1, 4))),
        "norm_gain": jnp.clip(1.0 + 0.18 * jax.random.normal(streams_of[1], (D,), jnp.float32), 0.1, 1.9),
        "w_query": gaussian(streams_of[2], (D, HEADS * HEAD_DIM), D ** -0.5, 0.125, ((0, 4), (1, 2))),
        "w_key": gaussian(streams_of[3], (D, KV_HEADS * HEAD_DIM), D ** -0.5, 0.125, ((0, 4), (1, 2))),
        "w_value": gaussian(streams_of[4], (D, KV_HEADS * HEAD_DIM), D ** -0.5, 0.125, ((0, 4), (1, 2))),
        "head_bias": jnp.clip(-1.5 + 2.5 * jax.random.uniform(streams_of[5], (HEADS,), jnp.float32) ** level_of(streams_of[5], (HEADS,), ((0, 2),), -0.2, 0.2), -1.5, 1.0),
        "cache_key": gaussian(streams_of[6], (SEQS, POS, KV_HEADS, HEAD_DIM), 1.0, 6.0, ((0, 4), (1, 4), (2, 2))),
        "cache_value": gaussian(streams_of[7], (SEQS, POS, KV_HEADS, HEAD_DIM), 1.0, 6.0, ((0, 4), (1, 4), (2, 2))),
        "lengths": place_ends(jax.random.randint(streams_of[8], (SEQS,), 1, POS), jax.random.fold_in(streams_of[8], 1), 1, POS - 1).astype(jnp.int32),
        "w_out": gaussian(streams_of[9], (HEADS * HEAD_DIM, D), (HEADS * HEAD_DIM) ** -0.5, 0.1875, ((0, 2), (1, 4))),
    }


norm_eps = 1e-06
out_eps = 1e-08

def reference(tokens, norm_gain, w_query, w_key, w_value, head_bias, cache_key, cache_value, lengths, w_out):
    floats_in = tokens.astype(jnp.float32)
    inv_rms = lax.rsqrt(lax.optimization_barrier(jnp.mean(floats_in * floats_in, axis=-1, keepdims=True)) + norm_eps)
    scaled = (floats_in * norm_gain).astype(jnp.bfloat16)
    queries = (inv_rms * jnp.dot(scaled, w_query, preferred_element_type=jnp.float32)).astype(jnp.bfloat16)
    new_key = (inv_rms * jnp.dot(scaled, w_key, preferred_element_type=jnp.float32)).astype(jnp.bfloat16)
    new_value = (inv_rms * jnp.dot(scaled, w_value, preferred_element_type=jnp.float32)).astype(jnp.bfloat16)
    group_size = HEADS // KV_HEADS
    queries = queries.reshape(SEQS, KV_HEADS, group_size, HEAD_DIM)
    offsets = (head_bias.astype(jnp.float32) - math.log(POS)).reshape(KV_HEADS, group_size, 1)
    positions = jnp.arange(POS, dtype=jnp.int32)

    def one_sequence(inputs):
        query_one, keys_one, values_one, length_one = inputs
        scores = jnp.einsum('cgd,pcd->cgp', query_one.astype(jnp.float32), keys_one.astype(jnp.float32), precision=lax.Precision.HIGHEST) * HEAD_DIM ** (-0.5) + offsets
        visible = (positions < length_one)[None, None, :]
        penalty = jnp.where(visible, jax.nn.softplus(scores), 0.0)
        between = lax.cumsum(penalty, axis=2, reverse=True) - penalty
        weights = jnp.where(visible, jnp.exp(jax.nn.log_sigmoid(scores) - between), 0.0)
        return jnp.einsum('cgp,pcd->cgd', weights, values_one.astype(jnp.float32), precision=lax.Precision.HIGHEST)
    attended = lax.map(one_sequence, (queries, cache_key, cache_value, lengths))
    attended = attended.reshape(SEQS, HEADS * HEAD_DIM)
    projected = jnp.dot(attended, w_out.astype(jnp.float32), preferred_element_type=jnp.float32, precision=lax.Precision.HIGHEST)
    mixed = projected * lax.rsqrt(lax.optimization_barrier(jnp.mean(projected * projected, axis=-1, keepdims=True)) + out_eps)
    return (mixed, new_key.reshape(SEQS, KV_HEADS, HEAD_DIM), new_value.reshape(SEQS, KV_HEADS, HEAD_DIM))
```

```python
import functools
import math

import jax
import jax.numpy as jnp
from jax import lax
from jax.experimental import pallas as pl
from jax.experimental.pallas import tpu as pltpu
from jax.sharding import PartitionSpec as P

norm_eps = 1e-06
out_eps = 1e-08
f32 = jnp.float32
bf16 = jnp.bfloat16
SUB = 8
LANES = 128


def kernel(
    dims,
    tok_hbm, gain_hbm, wq_hbm, wk_hbm, wv_hbm, bias_ref, ck_hbm, cv_hbm, len_ref, wo_hbm,
    mixed_ref, nk_ref, nv_ref,
    tok, gain, wq, wkv, ck, cv, wo,
    got_q, got_kv, got_att, got_tp, got_sq, qs, pen_s, ls_s, out_s, tot_s,
    load_sem, key_sem, val_sem,
    send_q, recv_q, send_kv, recv_kv, send_att, recv_att, send_tp, recv_tp, send_sq, recv_sq,
):
    n_kv, n_tp, seqs, heads, head_dim, pos_local, chunks = dims
    me = lax.axis_index("kv")
    me_tp = lax.axis_index("tp")
    groups = seqs // SUB
    width_local = tok.shape[1]
    full_width = width_local * n_kv
    all_pos = pos_local * n_kv

    loads = [
        pltpu.make_async_copy(tok_hbm, tok, load_sem.at[0]),
        pltpu.make_async_copy(gain_hbm, gain, load_sem.at[1]),
        pltpu.make_async_copy(wq_hbm, wq, load_sem.at[2]),
        pltpu.make_async_copy(wk_hbm, wkv.at[0], load_sem.at[3]),
        pltpu.make_async_copy(wv_hbm, wkv.at[1], load_sem.at[4]),
    ]
    for c in loads:
        c.start()
    per = seqs // chunks
    keys = [pltpu.make_async_copy(ck_hbm.at[pl.ds(i * per, per)], ck.at[pl.ds(i * per, per)], key_sem.at[i]) for i in range(chunks)]
    vals = [pltpu.make_async_copy(cv_hbm.at[pl.ds(i * per, per)], cv.at[pl.ds(i * per, per)], val_sem.at[i]) for i in range(chunks)]
    load_wo = pltpu.make_async_copy(wo_hbm, wo, load_sem.at[5])
    for c in keys + vals:
        c.start()
    load_wo.start()

    barrier = pltpu.get_barrier_semaphore()
    for d in range(1, n_kv):
        pl.semaphore_signal(barrier, inc=1, device_id={"kv": lax.rem(me + d, n_kv)}, device_id_type=pl.DeviceIdType.MESH)
    for d in range(1, n_tp):
        pl.semaphore_signal(barrier, inc=1, device_id={"tp": lax.rem(me_tp + d, n_tp)}, device_id_type=pl.DeviceIdType.MESH)

    def spread(buf, send, recv, axis, me_axis, n):
        copies = []
        for d in range(1, n):
            copies.append(pltpu.make_async_remote_copy(
                src_ref=buf.at[0], dst_ref=buf.at[d], send_sem=send.at[d - 1], recv_sem=recv.at[d - 1],
                device_id={axis: lax.rem(me_axis + d, n)}, device_id_type=pl.DeviceIdType.MESH))
        return copies

    def slot_of(source):
        return lax.rem(me - source + n_kv, n_kv)

    lane = lax.broadcasted_iota(jnp.int32, (SUB, LANES), 1)

    def pack(columns):
        tile = jnp.zeros((SUB, LANES), f32)
        for c, column in enumerate(columns):
            tile = jnp.where(lane == c, column, tile)
        return tile

    def unpack(tile, count):
        return [jnp.sum(jnp.where(lane == c, tile, 0.0), axis=1, keepdims=True) for c in range(count)]

    loads[0].wait()
    loads[1].wait()
    x = tok[...].astype(f32)
    squares = jnp.sum(x * x, axis=1, keepdims=True)
    scaled = (x * gain[...]).astype(bf16)
    loads[2].wait()
    part_q = jnp.dot(scaled, wq[...], preferred_element_type=f32)
    for h in range(heads):
        got_q[0, h * seqs:(h + 1) * seqs, :] = part_q[:, h * head_dim:(h + 1) * head_dim]
    got_q[0, heads * seqs:, :] = pack([squares[c * SUB:(c + 1) * SUB] for c in range(groups)])
    pl.semaphore_wait(barrier, n_kv - 1 + n_tp - 1)
    copies_q = spread(got_q, send_q, recv_q, "kv", me, n_kv)
    for c in copies_q:
        c.start()
    loads[3].wait()
    loads[4].wait()
    for i in range(2):
        got_kv[0, i * seqs:(i + 1) * seqs, :] = jnp.dot(scaled, wkv[i], preferred_element_type=f32)
    copies_kv = spread(got_kv, send_kv, recv_kv, "kv", me, n_kv)
    for c in copies_kv:
        c.start()

    later = lax.broadcasted_iota(jnp.int32, (pos_local, pos_local), 0) > lax.broadcasted_iota(jnp.int32, (pos_local, pos_local), 1)
    tri = jnp.where(later, 1.0, 0.0).astype(bf16)
    row = lax.broadcasted_iota(jnp.int32, (2 * heads, 1), 0)
    offset = jnp.zeros((2 * heads, 1), f32)
    for h in range(heads):
        offset = jnp.where(lax.rem(row, heads) == h, bias_ref[h], offset)
    offset = offset - math.log(all_pos)
    high = lax.broadcasted_iota(jnp.int32, (2 * heads, pos_local), 0) < heads
    positions = me * pos_local + lax.broadcasted_iota(jnp.int32, (2 * heads, pos_local), 1)

    for c in copies_q:
        c.wait_recv()
    sum_q = got_q[slot_of(0)]
    for k in range(1, n_kv):
        sum_q = sum_q + got_q[slot_of(k)]
    inv = [lax.rsqrt(t / full_width + norm_eps) for t in unpack(sum_q[heads * seqs:, :], groups)]
    inv = jnp.concatenate(inv, axis=0)
    stride = 2 * heads
    for h in range(heads):
        q = (sum_q[h * seqs:(h + 1) * seqs, :] * inv).astype(bf16).astype(f32)
        qs[pl.ds(h, seqs, stride=stride), :] = q
        qs[pl.ds(heads + h, seqs, stride=stride), :] = q

    for s in range(seqs):
        if s % per == 0:
            keys[s // per].wait()
        rows = slice(s * stride, (s + 1) * stride)
        score = lax.dot_general(qs[rows, :].astype(bf16), ck[s], (((1,), (1,)), ((), ())), preferred_element_type=f32)
        score = score * head_dim ** (-0.5) + offset
        tail = jnp.log1p(jnp.exp(-jnp.abs(score)))
        visible = positions < len_ref[s]
        penalty = jnp.where(visible, jnp.maximum(score, 0.0) + tail, 0.0)
        top = penalty.astype(bf16).astype(f32)
        pen_s[rows, :] = jnp.where(high, top, penalty - top)
        ls_s[rows, :] = jnp.where(visible, jnp.minimum(score, 0.0) - tail, -1e30)
    suffix = jnp.dot(pen_s[...].astype(bf16), tri, preferred_element_type=f32)
    for s in range(seqs):
        if s % per == 0:
            vals[s // per].wait()
        rows = slice(s * stride, (s + 1) * stride)
        between = suffix[rows, :]
        between = between + pltpu.roll(between, heads, 0)
        weights = jnp.exp(ls_s[rows, :] - between)
        top = weights.astype(bf16).astype(f32)
        parts = jnp.where(high, top, weights - top).astype(bf16)
        out = jnp.dot(parts, cv[s], preferred_element_type=f32)
        out_s[rows, :] = out + pltpu.roll(out, heads, 0)
        first = pen_s[rows, 0:LANES]
        total = between[:, 0:LANES] + first + pltpu.roll(first, heads, 0)
        tot_s[rows, :] = total
    columns = []
    for h in range(heads):
        got_att[0, h * seqs:(h + 1) * seqs, :] = out_s[pl.ds(h, seqs, stride=stride), :]
        totals = tot_s[pl.ds(h, seqs, stride=stride), :]
        columns += [totals[c * SUB:(c + 1) * SUB, 0:1] for c in range(groups)]
    got_att[0, heads * seqs:, :] = pack(columns)
    copies_att = spread(got_att, send_att, recv_att, "kv", me, n_kv)
    for c in copies_att:
        c.start()

    for c in copies_kv:
        c.wait_recv()
    sum_kv = got_kv[slot_of(0)]
    for k in range(1, n_kv):
        sum_kv = sum_kv + got_kv[slot_of(k)]
    nk_ref[...] = (sum_kv[:seqs, :] * inv).astype(bf16)
    nv_ref[...] = (sum_kv[seqs:, :] * inv).astype(bf16)
    load_wo.wait()

    for c in copies_att:
        c.wait_recv()
    pieces = [None] * heads
    behind = jnp.zeros((SUB, LANES), f32)
    for k in reversed(range(n_kv)):
        slot = slot_of(k)
        factor = jnp.exp(-behind)
        behind = behind + got_att[slot, heads * seqs:, :]
        for h in range(heads):
            f = jnp.concatenate([factor[:, h * groups + c:h * groups + c + 1] for c in range(groups)], axis=0)
            term = got_att[slot, h * seqs:(h + 1) * seqs, :] * f
            pieces[h] = term if pieces[h] is None else pieces[h] + term
    attended = jnp.concatenate(pieces, axis=1)
    top = attended.astype(bf16).astype(f32)
    both = jnp.concatenate([top, attended - top], axis=0).astype(bf16)
    partial = jnp.dot(both, wo[...], preferred_element_type=f32)
    got_tp[0] = partial[:seqs, :] + partial[seqs:, :]
    copies_tp = spread(got_tp, send_tp, recv_tp, "tp", me_tp, n_tp)
    for c in copies_tp:
        c.start()
    for c in copies_tp:
        c.wait_recv()
    projected = got_tp[lax.rem(me_tp + n_tp, n_tp)]
    for k in range(1, n_tp):
        projected = projected + got_tp[lax.rem(me_tp - k + n_tp, n_tp)]
    squares = jnp.sum(projected * projected, axis=1, keepdims=True)
    got_sq[0] = pack([squares[c * SUB:(c + 1) * SUB] for c in range(groups)])
    copies_sq = spread(got_sq, send_sq, recv_sq, "kv", me, n_kv)
    for c in copies_sq:
        c.start()
    for c in copies_sq:
        c.wait_recv()
    total = got_sq[slot_of(0)]
    for k in range(1, n_kv):
        total = total + got_sq[slot_of(k)]
    scale = [lax.rsqrt(t / full_width + out_eps) for t in unpack(total, groups)]
    mixed_ref[...] = projected * jnp.concatenate(scale, axis=0)
    for c in copies_q + copies_kv + copies_att + copies_tp + copies_sq:
        c.wait_send()


def body(
    tokens, norm_gain, w_query, w_key, w_value, head_bias, cache_key, cache_value, lengths, w_out
):
    n_kv, n_tp = lax.axis_size("kv"), lax.axis_size("tp")
    seqs, width_local = tokens.shape
    pos_local, kv_local, head_dim = cache_key.shape[1:]
    heads = head_bias.shape[0]
    out_local = w_out.shape[1]
    chunks = 3 if seqs % 3 == 0 else 1
    assert kv_local == 1 and head_dim == LANES and 2 * heads == SUB and seqs % SUB == 0
    assert heads * (seqs // SUB) <= LANES
    dims = (n_kv, n_tp, seqs, heads, head_dim, pos_local, chunks)
    q_rows = heads * seqs + SUB
    rows = 2 * heads * seqs
    any_spec = pl.BlockSpec(memory_space=pl.ANY)
    smem = pl.BlockSpec(memory_space=pltpu.SMEM)
    vmem = pl.BlockSpec(memory_space=pltpu.VMEM)
    dma = pltpu.SemaphoreType.DMA
    kv_sems = [dma((n_kv - 1,))] * 2
    mixed, new_key, new_value = pl.pallas_call(
        functools.partial(kernel, dims),
        out_shape=(
            jax.ShapeDtypeStruct((seqs, out_local), f32),
            jax.ShapeDtypeStruct((seqs, head_dim), bf16),
            jax.ShapeDtypeStruct((seqs, head_dim), bf16),
        ),
        in_specs=[any_spec] * 5 + [smem] + [any_spec] * 2 + [smem] + [any_spec],
        out_specs=[vmem] * 3,
        scratch_shapes=[
            pltpu.VMEM((seqs, width_local), bf16),
            pltpu.VMEM((1, width_local), f32),
            pltpu.VMEM(w_query.shape, bf16),
            pltpu.VMEM((2,) + w_key.shape, bf16),
            pltpu.VMEM((seqs, pos_local, head_dim), bf16),
            pltpu.VMEM((seqs, pos_local, head_dim), bf16),
            pltpu.VMEM(w_out.shape, bf16),
            pltpu.VMEM((n_kv, q_rows, LANES), f32),
            pltpu.VMEM((n_kv, 2 * seqs, LANES), f32),
            pltpu.VMEM((n_kv, q_rows, LANES), f32),
            pltpu.VMEM((n_tp, seqs, out_local), f32),
            pltpu.VMEM((n_kv, SUB, LANES), f32),
            pltpu.VMEM((rows, head_dim), f32),
            pltpu.VMEM((rows, pos_local), f32),
            pltpu.VMEM((rows, pos_local), f32),
            pltpu.VMEM((rows, head_dim), f32),
            pltpu.VMEM((rows, LANES), f32),
            dma((6,)), dma((chunks,)), dma((chunks,)),
            *kv_sems, *kv_sems, *kv_sems,
            dma((max(n_tp - 1, 1),)), dma((max(n_tp - 1, 1),)),
            *kv_sems,
        ],
        compiler_params=pltpu.CompilerParams(collective_id=0, has_side_effects=True),
    )(
        tokens, norm_gain.reshape(1, width_local), w_query, w_key, w_value, head_bias,
        cache_key.reshape(seqs, pos_local, head_dim), cache_value.reshape(seqs, pos_local, head_dim),
        lengths, w_out,
    )
    return (
        mixed,
        new_key.reshape(seqs, kv_local, head_dim),
        new_value.reshape(seqs, kv_local, head_dim),
    )


def solution(mesh):
    placed = (
        P("dp", "kv"),
        P("kv"),
        P("kv", "tp"),
        P("kv", "tp"),
        P("kv", "tp"),
        P("tp"),
        P("dp", "kv", "tp", None),
        P("dp", "kv", "tp", None),
        P("dp"),
        P("tp", "kv"),
    )
    return jax.shard_map(
        body,
        mesh=mesh,
        in_specs=placed,
        out_specs=(P("dp", "kv"), P("dp", "tp", None), P("dp", "tp", None)),
        check_vma=False,
    )
```

```python
import functools
import math

import jax
import jax.numpy as jnp
from jax import lax
from jax.experimental import pallas as pl
from jax.experimental.pallas import tpu as pltpu
from jax.sharding import PartitionSpec as P

norm_eps = 1e-06
out_eps = 1e-08
f32 = jnp.float32
bf16 = jnp.bfloat16
SUB = 8
LANES = 128


def kernel(
    dims,
    tok_hbm, gain_hbm, wq_hbm, wk_hbm, wv_hbm, bias_ref, ck_hbm, cv_hbm, len_ref, wo_hbm,
    mixed_ref, nk_ref, nv_ref,
    tok, gain, wq, wkv, ck, cv, wo,
    got_q, got_kv, got_att, got_tp, got_sq, qs, pen_s, ls_s, out_s, tot_s, tri,
    load_sem, key_sem, val_sem,
    send_q, recv_q, send_kv, recv_kv, send_att, recv_att, send_tp, recv_tp, send_sq, recv_sq,
):
    n_kv, n_tp, seqs, heads, head_dim, pos_local, chunks = dims
    me = lax.axis_index("kv")
    me_tp = lax.axis_index("tp")
    groups = seqs // SUB
    width_local = tok.shape[1]
    full_width = width_local * n_kv
    all_pos = pos_local * n_kv

    loads = [
        pltpu.make_async_copy(tok_hbm, tok, load_sem.at[0]),
        pltpu.make_async_copy(gain_hbm, gain, load_sem.at[1]),
        pltpu.make_async_copy(wq_hbm, wq, load_sem.at[2]),
        pltpu.make_async_copy(wk_hbm, wkv.at[0], load_sem.at[3]),
        pltpu.make_async_copy(wv_hbm, wkv.at[1], load_sem.at[4]),
    ]
    for c in loads:
        c.start()
    per = seqs // chunks
    keys = [pltpu.make_async_copy(ck_hbm.at[pl.ds(i * per, per)], ck.at[pl.ds(i * per, per)], key_sem.at[i]) for i in range(chunks)]
    vals = [pltpu.make_async_copy(cv_hbm.at[pl.ds(i * per, per)], cv.at[pl.ds(i * per, per)], val_sem.at[i]) for i in range(chunks)]
    load_wo = pltpu.make_async_copy(wo_hbm, wo, load_sem.at[5])
    for c in keys + vals:
        c.start()
    load_wo.start()

    barrier = pltpu.get_barrier_semaphore()
    for d in range(1, n_kv):
        pl.semaphore_signal(barrier, inc=1, device_id={"kv": lax.rem(me + d, n_kv)}, device_id_type=pl.DeviceIdType.MESH)
    for d in range(1, n_tp):
        pl.semaphore_signal(barrier, inc=1, device_id={"tp": lax.rem(me_tp + d, n_tp)}, device_id_type=pl.DeviceIdType.MESH)

    def spread(buf, rows, send, recv, first, axis, me_axis, n):
        copies = []
        for d in range(1, n):
            at = first * (n - 1) + d - 1
            copies.append(pltpu.make_async_remote_copy(
                src_ref=buf.at[0, rows], dst_ref=buf.at[d, rows], send_sem=send.at[at], recv_sem=recv.at[at],
                device_id={axis: lax.rem(me_axis + d, n)}, device_id_type=pl.DeviceIdType.MESH))
            copies[-1].start()
        return copies

    def slot_of(source):
        return lax.rem(me - source + n_kv, n_kv)

    lane = lax.broadcasted_iota(jnp.int32, (SUB, LANES), 1)

    def pack(columns):
        tile = jnp.zeros((SUB, LANES), f32)
        for c, column in enumerate(columns):
            tile = jnp.where(lane == c, column, tile)
        return tile

    def unpack(tile, count):
        return [jnp.sum(jnp.where(lane == c, tile, 0.0), axis=1, keepdims=True) for c in range(count)]

    loads[0].wait()
    loads[1].wait()
    x = tok[...].astype(f32)
    squares = jnp.sum(x * x, axis=1, keepdims=True)
    scaled = (x * gain[...]).astype(bf16)
    loads[2].wait()
    part_q = jnp.dot(scaled, wq[...], preferred_element_type=f32)
    block = heads * SUB
    got_q[0, :SUB, :] = pack([squares[g * SUB:(g + 1) * SUB] for g in range(groups)])
    for g in range(groups):
        for h in range(heads):
            at = SUB + g * block + h * SUB
            got_q[0, at:at + SUB, :] = part_q[g * SUB:(g + 1) * SUB, h * head_dim:(h + 1) * head_dim]
    pl.semaphore_wait(barrier, n_kv - 1 + n_tp - 1)
    copies_q = []
    for g in range(groups):
        rows = pl.ds(0, SUB + block) if g == 0 else pl.ds(SUB + g * block, block)
        copies_q.append(spread(got_q, rows, send_q, recv_q, g, "kv", me, n_kv))

    later = lax.broadcasted_iota(jnp.int32, (pos_local, pos_local), 0) > lax.broadcasted_iota(jnp.int32, (pos_local, pos_local), 1)
    tri[...] = jnp.where(later, 1.0, 0.0).astype(bf16)
    row = lax.broadcasted_iota(jnp.int32, (2 * heads, 1), 0)
    offset = jnp.zeros((2 * heads, 1), f32)
    for h in range(heads):
        offset = jnp.where(lax.rem(row, heads) == h, bias_ref[h], offset)
    offset = offset - math.log(all_pos)
    high = lax.broadcasted_iota(jnp.int32, (2 * heads, pos_local), 0) < heads
    positions = me * pos_local + lax.broadcasted_iota(jnp.int32, (2 * heads, pos_local), 1)
    loads[3].wait()
    loads[4].wait()
    for i in range(2):
        got_kv[0, i * seqs:(i + 1) * seqs, :] = jnp.dot(scaled, wkv[i], preferred_element_type=f32)

    stride = 2 * heads
    inv = None
    copies_att = []
    for g in range(groups):
        for c in copies_q[g]:
            c.wait_recv()
        rows = slice(0, SUB + block) if g == 0 else slice(SUB + g * block, SUB + (g + 1) * block)
        sum_q = got_q[slot_of(0), rows, :]
        for k in range(1, n_kv):
            sum_q = sum_q + got_q[slot_of(k), rows, :]
        if g == 0:
            inv = [lax.rsqrt(t / full_width + norm_eps) for t in unpack(sum_q[:SUB, :], groups)]
            sum_q = sum_q[SUB:, :]
        base = g * SUB * stride
        for h in range(heads):
            q = (sum_q[h * SUB:(h + 1) * SUB, :] * inv[g]).astype(bf16).astype(f32)
            qs[pl.ds(base + h, SUB, stride=stride), :] = q
            qs[pl.ds(base + heads + h, SUB, stride=stride), :] = q
        keys[g].wait()
        for s in range(g * SUB, (g + 1) * SUB):
            rows = slice(s * stride, (s + 1) * stride)
            score = lax.dot_general(qs[rows, :].astype(bf16), ck[s], (((1,), (1,)), ((), ())), preferred_element_type=f32)
            score = score * head_dim ** (-0.5) + offset
            tail = jnp.log1p(jnp.exp(-jnp.abs(score)))
            visible = positions < len_ref[s]
            penalty = jnp.where(visible, jnp.maximum(score, 0.0) + tail, 0.0)
            top = penalty.astype(bf16).astype(f32)
            pen_s[rows, :] = jnp.where(high, top, penalty - top)
            ls_s[rows, :] = jnp.where(visible, jnp.minimum(score, 0.0) - tail, -1e30)
        suffix = jnp.dot(pen_s[base:base + SUB * stride, :].astype(bf16), tri[...], preferred_element_type=f32)
        vals[g].wait()
        for s in range(g * SUB, (g + 1) * SUB):
            rows = slice(s * stride, (s + 1) * stride)
            between = suffix[s * stride - base:(s + 1) * stride - base, :]
            between = between + pltpu.roll(between, heads, 0)
            weights = jnp.exp(ls_s[rows, :] - between)
            top = weights.astype(bf16).astype(f32)
            parts = jnp.where(high, top, weights - top).astype(bf16)
            out = jnp.dot(parts, cv[s], preferred_element_type=f32)
            out_s[rows, :] = out + pltpu.roll(out, heads, 0)
            first = pen_s[rows, 0:LANES]
            tot_s[rows, :] = between[:, 0:LANES] + first + pltpu.roll(first, heads, 0)
        columns = []
        at = g * (block + SUB)
        for h in range(heads):
            got_att[0, at + h * SUB:at + (h + 1) * SUB, :] = out_s[pl.ds(base + h, SUB, stride=stride), :]
            columns.append(tot_s[pl.ds(base + h, SUB, stride=stride), :][:, 0:1])
        got_att[0, at + block:at + block + SUB, :] = pack(columns)
        copies_att.append(spread(got_att, pl.ds(at, block + SUB), send_att, recv_att, g, "kv", me, n_kv))
    copies_kv = spread(got_kv, pl.ds(0, 2 * seqs), send_kv, recv_kv, 0, "kv", me, n_kv)
    load_wo.wait()

    copies_tp = []
    for g in range(groups):
        for c in copies_att[g]:
            c.wait_recv()
        at = g * (block + SUB)
        pieces = [None] * heads
        behind = jnp.zeros((SUB, LANES), f32)
        for k in reversed(range(n_kv)):
            slot = slot_of(k)
            factor = jnp.exp(-behind)
            behind = behind + got_att[slot, at + block:at + block + SUB, :]
            for h in range(heads):
                term = got_att[slot, at + h * SUB:at + (h + 1) * SUB, :] * factor[:, h:h + 1]
                pieces[h] = term if pieces[h] is None else pieces[h] + term
        attended = jnp.concatenate(pieces, axis=1)
        top = attended.astype(bf16).astype(f32)
        both = jnp.concatenate([top, attended - top], axis=0).astype(bf16)
        partial = jnp.dot(both, wo[...], preferred_element_type=f32)
        got_tp[0, g * SUB:(g + 1) * SUB, :] = partial[:SUB, :] + partial[SUB:, :]
        copies_tp.append(spread(got_tp, pl.ds(g * SUB, SUB), send_tp, recv_tp, g, "tp", me_tp, n_tp))
    projected = []
    columns = []
    for g in range(groups):
        for c in copies_tp[g]:
            c.wait_recv()
        rows = slice(g * SUB, (g + 1) * SUB)
        p = got_tp[lax.rem(me_tp + n_tp, n_tp), rows, :]
        for k in range(1, n_tp):
            p = p + got_tp[lax.rem(me_tp - k + n_tp, n_tp), rows, :]
        projected.append(p)
        columns.append(jnp.sum(p * p, axis=1, keepdims=True))
    got_sq[0] = pack(columns)
    copies_sq = spread(got_sq, pl.ds(0, SUB), send_sq, recv_sq, 0, "kv", me, n_kv)

    for c in copies_kv:
        c.wait_recv()
    sum_kv = got_kv[slot_of(0)]
    for k in range(1, n_kv):
        sum_kv = sum_kv + got_kv[slot_of(k)]
    inv = jnp.concatenate(inv, axis=0)
    nk_ref[...] = (sum_kv[:seqs, :] * inv).astype(bf16)
    nv_ref[...] = (sum_kv[seqs:, :] * inv).astype(bf16)

    for c in copies_sq:
        c.wait_recv()
    total = got_sq[slot_of(0)]
    for k in range(1, n_kv):
        total = total + got_sq[slot_of(k)]
    scale = [lax.rsqrt(t / full_width + out_eps) for t in unpack(total, groups)]
    for g in range(groups):
        mixed_ref[g * SUB:(g + 1) * SUB, :] = projected[g] * scale[g]
    for c in sum(copies_q + copies_att + copies_tp, []) + copies_kv + copies_sq:
        c.wait_send()


def body(
    tokens, norm_gain, w_query, w_key, w_value, head_bias, cache_key, cache_value, lengths, w_out
):
    n_kv, n_tp = lax.axis_size("kv"), lax.axis_size("tp")
    seqs, width_local = tokens.shape
    pos_local, kv_local, head_dim = cache_key.shape[1:]
    heads = head_bias.shape[0]
    out_local = w_out.shape[1]
    chunks = seqs // SUB
    assert kv_local == 1 and head_dim == LANES and 2 * heads == SUB and seqs % SUB == 0
    assert heads * (seqs // SUB) <= LANES
    dims = (n_kv, n_tp, seqs, heads, head_dim, pos_local, chunks)
    q_rows = heads * seqs + SUB
    att_rows = heads * seqs + chunks * SUB
    rows = 2 * heads * seqs
    any_spec = pl.BlockSpec(memory_space=pl.ANY)
    smem = pl.BlockSpec(memory_space=pltpu.SMEM)
    vmem = pl.BlockSpec(memory_space=pltpu.VMEM)
    dma = pltpu.SemaphoreType.DMA
    one = [dma((n_kv - 1,))] * 2
    each = [dma(((n_kv - 1) * chunks,))] * 2
    across = [dma((max(n_tp - 1, 1) * chunks,))] * 2
    mixed, new_key, new_value = pl.pallas_call(
        functools.partial(kernel, dims),
        out_shape=(
            jax.ShapeDtypeStruct((seqs, out_local), f32),
            jax.ShapeDtypeStruct((seqs, head_dim), bf16),
            jax.ShapeDtypeStruct((seqs, head_dim), bf16),
        ),
        in_specs=[any_spec] * 5 + [smem] + [any_spec] * 2 + [smem] + [any_spec],
        out_specs=[vmem] * 3,
        scratch_shapes=[
            pltpu.VMEM((seqs, width_local), bf16),
            pltpu.VMEM((1, width_local), f32),
            pltpu.VMEM(w_query.shape, bf16),
            pltpu.VMEM((2,) + w_key.shape, bf16),
            pltpu.VMEM((seqs, pos_local, head_dim), bf16),
            pltpu.VMEM((seqs, pos_local, head_dim), bf16),
            pltpu.VMEM(w_out.shape, bf16),
            pltpu.VMEM((n_kv, q_rows, LANES), f32),
            pltpu.VMEM((n_kv, 2 * seqs, LANES), f32),
            pltpu.VMEM((n_kv, att_rows, LANES), f32),
            pltpu.VMEM((n_tp, seqs, out_local), f32),
            pltpu.VMEM((n_kv, SUB, LANES), f32),
            pltpu.VMEM((rows, head_dim), f32),
            pltpu.VMEM((rows, pos_local), f32),
            pltpu.VMEM((rows, pos_local), f32),
            pltpu.VMEM((rows, head_dim), f32),
            pltpu.VMEM((rows, LANES), f32),
            pltpu.VMEM((pos_local, pos_local), bf16),
            dma((6,)), dma((chunks,)), dma((chunks,)),
            *each, *one, *each, *across, *one,
        ],
        compiler_params=pltpu.CompilerParams(collective_id=0, has_side_effects=True),
    )(
        tokens, norm_gain.reshape(1, width_local), w_query, w_key, w_value, head_bias,
        cache_key.reshape(seqs, pos_local, head_dim), cache_value.reshape(seqs, pos_local, head_dim),
        lengths, w_out,
    )
    return (
        mixed,
        new_key.reshape(seqs, kv_local, head_dim),
        new_value.reshape(seqs, kv_local, head_dim),
    )


def solution(mesh):
    placed = (
        P("dp", "kv"),
        P("kv"),
        P("kv", "tp"),
        P("kv", "tp"),
        P("kv", "tp"),
        P("tp"),
        P("dp", "kv", "tp", None),
        P("dp", "kv", "tp", None),
        P("dp"),
        P("tp", "kv"),
    )
    return jax.shard_map(
        body,
        mesh=mesh,
        in_specs=placed,
        out_specs=(P("dp", "kv"), P("dp", "tp", None), P("dp", "tp", None)),
        check_vma=False,
    )
```
